128 devices in a mesh: sp: 64 (over z, y, x), tp: 2 (over core).
Axes of the slice: x: 4, y: 4, z: 4, core: 2. Of those that a mesh axis runs over, the one named last changes fastest.
Arguments:
- tokens: bfloat16 [32768, 4096], P(('sp', 'tp')), may hold values from -6 to 6
- norm_gain: float32 [4096], replicated, may hold values from 0.5 to 1.5
- query_weight: bfloat16 [4096, 1024], P(None, 'tp'), may hold values from -0.09375 to 0.09375
- key_weight: bfloat16 [4096, 1024], P(None, 'tp'), may hold values from -0.09375 to 0.09375
- value_weight: bfloat16 [4096, 2048], P(None, 'tp'), may hold values from -0.09375 to 0.09375
- gate_weight: bfloat16 [4096, 2048], P(None, 'tp'), may hold values from -0.09375 to 0.09375
- decay_bias: float32 [1024], P('tp'), may hold values from -0.5 to 0.5
- head_gain: float32 [2048], P('tp'), may hold values from 0.5 to 1.5
- out_weight: bfloat16 [2048, 4096], P('tp'), may hold values from -0.125 to 0.125
Outputs:
- layer_out: bfloat16 [32768, 4096], P(('sp', 'tp'))
The draws below stay inside these ranges and needn't reach their ends.
All inputs are finite; a program needn't handle non-finite values.
Results may differ from the reference program's by a relative error of at most 0.015.
Values may be sent and summed in bfloat16 or wider, within the bound.
A program may use at most 192 MiB of HBM per device.

```python
import math
import jax
import jax.numpy as jnp
from jax import lax

D = 4096
HEADS = 8
HEAD_K = 128
HEAD_V = 256
BLOCK = 64
SEQ = 32768
KEY_DIM = 1024
VALUE_DIM = 2048


def level_of(own_key, dims, cuts, least, top_value):
    level, own = 1.0, jax.random.fold_in(own_key, 6)
    for axis_at, shards_of in cuts:
        steps = jnp.exp(jax.random.uniform(jax.random.fold_in(own, axis_at), (shards_of,), jnp.float32, least / len(cuts), top_value / len(cuts)))
        level = level * jnp.repeat(steps, dims[axis_at] // shards_of).reshape([-1 if axis == axis_at else 1 for axis in range(len(dims))])
    return level


def bell_draw(rng, extent, spread, reach, shards=(), kind=jnp.bfloat16):
    gain = level_of(rng, extent, shards, -0.22, 0.18) if shards else 1.0
    array = jax.random.normal(rng, extent, jnp.float32) * spread * gain
    return jnp.minimum(jnp.maximum(array, -reach), reach).astype(kind)


def setup_inputs(seed: int = 0) -> dict:
    key_list = jax.random.split(jax.random.key(seed), 10)
    tokens = bell_draw(key_list[0], (SEQ, D), 1.0, 6.0, ((0, 128),))
    norm_gain = jnp.clip(1.0 + 0.1 * jax.random.normal(key_list[1], (D,), jnp.float32), 0.5, 1.5)
    query_weight = bell_draw(key_list[2], (D, KEY_DIM), D ** -0.5, 0.09375, ((1, 2),))
    key_weight = bell_draw(key_list[3], (D, KEY_DIM), D ** -0.5, 0.09375, ((1, 2),))
    value_weight = bell_draw(key_list[4], (D, VALUE_DIM), D ** -0.5, 0.09375, ((1, 2),))
    gate_weight = bell_draw(key_list[5], (D, VALUE_DIM), D ** -0.5, 0.09375, ((1, 2),))
    decay_bias = jnp.clip(jax.random.uniform(key_list[6], (KEY_DIM,), jnp.float32, -0.5, 0.5) * level_of(key_list[6], (KEY_DIM,), ((0, 2),), -0.4, 0.0), -0.5, 0.5)
    head_gain = jnp.clip(1.0 + 0.1 * jax.random.normal(key_list[7], (VALUE_DIM,), jnp.float32), 0.5, 1.5)
    out_weight = bell_draw(key_list[8], (VALUE_DIM, D), VALUE_DIM ** -0.5, 0.125, ((0, 2),))
    return {"tokens": tokens, "norm_gain": norm_gain, "query_weight": query_weight, "key_weight": key_weight, "value_weight": value_weight, "gate_weight": gate_weight, "decay_bias": decay_bias, "head_gain": head_gain, "out_weight": out_weight}


epsilon = 1e-06
decay_power = 16.0
precise = lax.Precision.HIGHEST

def to_blocks(values, head_count, head_width):
    block_count = values.shape[0] // BLOCK
    return values.astype(jnp.float32).reshape(block_count, BLOCK, head_count, head_width).transpose(0, 2, 1, 3)

def reference(tokens, norm_gain, query_weight, key_weight, value_weight, gate_weight, decay_bias, head_gain, out_weight):
    inputs = tokens.astype(jnp.float32)
    row_scale = lax.rsqrt(lax.optimization_barrier(jnp.mean(inputs * inputs, axis=-1, keepdims=True)) + epsilon)
    normed = (inputs * row_scale * norm_gain.astype(jnp.float32)).astype(jnp.bfloat16)
    query_rows = jnp.dot(normed, query_weight, preferred_element_type=jnp.float32).astype(jnp.bfloat16)
    key_rows = jnp.dot(normed, key_weight, preferred_element_type=jnp.float32).astype(jnp.bfloat16)
    value_rows = jnp.dot(normed, value_weight, preferred_element_type=jnp.float32).astype(jnp.bfloat16)
    gate_input = jnp.dot(normed, gate_weight, preferred_element_type=jnp.float32).astype(jnp.bfloat16)
    logits = decay_bias.astype(jnp.float32) + math.log(SEQ / 8.0)
    log_decay = jnp.broadcast_to(jax.nn.log_sigmoid(logits) / decay_power, (SEQ, KEY_DIM))
    query_blocks = to_blocks(query_rows, HEADS, HEAD_K) * HEAD_K ** (-0.5)
    key_blocks = to_blocks(key_rows, HEADS, HEAD_K)
    value_blocks = to_blocks(value_rows, HEADS, HEAD_V)
    decay_blocks = to_blocks(log_decay, HEADS, HEAD_K)
    within = jnp.cumsum(decay_blocks, axis=2)
    block_end = within[:, :, -1:, :]
    query_in = query_blocks * jnp.exp(within)
    key_in = key_blocks * jnp.exp(-within)
    key_out = key_blocks * jnp.exp(block_end - within)
    causal = jnp.tril(jnp.ones((BLOCK, BLOCK), dtype=bool))
    scores = jnp.where(causal, jnp.einsum('nhid,nhjd->nhij', query_in, key_in, precision=precise), 0.0)
    local_out = jnp.einsum('nhij,nhjv->nhiv', scores, value_blocks, precision=precise)
    block_decay = jnp.exp(block_end[:, :, 0, :])

    def advance(carry_state, inputs_now):
        query_now, key_now, value_now, decay_now = inputs_now
        carried = jnp.einsum('hid,hdv->hiv', query_now, carry_state, precision=precise)
        carry_state = decay_now[..., None] * carry_state + jnp.einsum('hjd,hjv->hdv', key_now, value_now, precision=precise)
        return (carry_state, carried)
    start_state = jnp.zeros((HEADS, HEAD_K, HEAD_V), jnp.float32)
    _, carried_out = lax.scan(advance, start_state, (query_in, key_out, value_blocks, block_decay))
    mixed_heads = (local_out + carried_out).transpose(0, 2, 1, 3).reshape(SEQ, HEADS, HEAD_V)
    head_scale = lax.rsqrt(lax.optimization_barrier(jnp.mean(mixed_heads * mixed_heads, axis=-1, keepdims=True)) + epsilon)
    normed_heads = (mixed_heads * head_scale * head_gain.astype(jnp.float32).reshape(HEADS, HEAD_V)).reshape(SEQ, HEADS * HEAD_V)
    gated_rows = (normed_heads * jax.nn.silu(gate_input.astype(jnp.float32))).astype(jnp.bfloat16)
    return jnp.dot(gated_rows, out_weight, preferred_element_type=jnp.float32).astype(jnp.bfloat16)
```

```python
import functools
import math
import types

import jax
import jax.numpy as jnp
from jax import lax
from jax.experimental import pallas as pl
from jax.experimental.pallas import tpu as pltpu
from jax.sharding import PartitionSpec as P

HEAD_K = 128
HEAD_V = 256
PIECES = 16
PIECE_ROWS = 16
LANES = 128

epsilon = 1e-06
decay_power = 16.0
MESH = pl.DeviceIdType.MESH
f32 = jnp.float32
bf16 = jnp.bfloat16
OUT_TILE = 512
TOKEN_CHUNKS = 4
VMEM_BYTES = 67_000_000


def nn(a, b):
    return jnp.dot(a, b, preferred_element_type=f32)


def nt(a, b):
    return lax.dot_general(a, b, (((1,), (1,)), ((), ())), preferred_element_type=f32)


def tn(a, b):
    return lax.dot_general(a, b, (((0,), (0,)), ((), ())), preferred_element_type=f32)


def mark(name):
    pass


def kernel(sp_count, names, *refs):
    r = types.SimpleNamespace(**dict(zip(names, refs, strict=True)))
    s = lax.axis_index("sp")
    c = lax.axis_index("tp")
    other = 1 - c
    half, model = r.tokens.shape
    span = 2 * half
    heads = r.wk.shape[1] // HEAD_K
    groups = 2
    pair = heads // groups
    vcols = pair * HEAD_V
    inner = PIECES
    outer = sp_count // inner
    z = s // inner
    p = lax.rem(s, inner)

    own = pl.ds(pl.multiple_of(c * half, half), half)
    theirs = pl.ds(pl.multiple_of(other * half, half), half)
    partner = {"sp": s, "tp": other}

    def plane_dev(i):
        return {"sp": z * inner + i, "tp": c}

    def outer_dev(k):
        return {"sp": k * inner + p, "tp": c}

    def remote(src, dst, ssem, rsem, device):
        return pltpu.make_async_remote_copy(
            src_ref=src,
            dst_ref=dst,
            send_sem=ssem,
            recv_sem=rsem,
            device_id=device,
            device_id_type=MESH,
        )

    chunk = half // TOKEN_CHUNKS
    tok_copies = []
    for i in range(TOKEN_CHUNKS):
        rows = pl.ds(i * chunk, chunk)
        mine = pl.ds(pl.multiple_of(c * half + i * chunk, chunk), chunk)
        tok_copies.append(
            pltpu.make_async_copy(r.tokens.at[rows, :], r.xn.at[mine, :], r.tok_sem.at[i])
        )
    small = [
        pltpu.make_async_copy(r.norm_gain, r.gain_v, r.small_sem.at[0]),
        pltpu.make_async_copy(r.decay_bias, r.bias_v, r.small_sem.at[1]),
        pltpu.make_async_copy(r.head_gain, r.hgain_v, r.small_sem.at[2]),
    ]
    wk_copy = pltpu.make_async_copy(r.wk, r.wk_v, r.w_sem.at[0])
    wq_copy = pltpu.make_async_copy(r.wq, r.wq_v, r.w_sem.at[1])
    wv_copies, wg_copies = [], []
    for g in range(groups):
        cols = pl.ds(g * vcols, vcols)
        wv_copies.append(
            pltpu.make_async_copy(r.wv.at[:, cols], r.wv_v.at[:, cols], r.w_sem.at[2 + g])
        )
        wg_copies.append(
            pltpu.make_async_copy(
                r.wg.at[:, cols], r.wg_v.at[:, cols], r.w_sem.at[2 + groups + g]
            )
        )
    wo_copy = pltpu.make_async_copy(r.wo, r.wo_v, r.wo_sem)
    tok_copies[0].start()
    small[0].start()
    for copy in tok_copies[1:]:
        copy.start()
    for copy in [wk_copy] + wv_copies + [wq_copy] + small[1:] + wg_copies + [wo_copy]:
        copy.start()

    barrier = pltpu.get_barrier_semaphore()
    pl.semaphore_signal(barrier, inc=1, device_id=partner, device_id_type=MESH)
    for d in range(1, inner):
        pl.semaphore_signal(
            barrier, inc=1, device_id=plane_dev(lax.rem(p + d, inner)), device_id_type=MESH
        )
    for d in range(1, outer):
        pl.semaphore_signal(
            barrier, inc=1, device_id=outer_dev(lax.rem(z + d, outer)), device_id_type=MESH
        )

    mark("p_norm")
    sub = 16
    small[0].wait()
    for i in range(TOKEN_CHUNKS):
        tok_copies[i].wait()
        first = c * half + i * chunk

        @pl.loop(0, chunk // sub, unroll=True)
        def _(k):
            rows = pl.ds(pl.multiple_of(first + k * sub, sub), sub)
            x = r.xn[rows, :].astype(f32)
            scale = lax.rsqrt(jnp.mean(x * x, axis=-1, keepdims=True) + epsilon)
            r.scale_v[pl.ds(k * sub, sub), :] = jnp.broadcast_to(scale, (sub, LANES))

        @pl.loop(0, chunk // sub)
        def _(k):
            rows = pl.ds(pl.multiple_of(first + k * sub, sub), sub)
            x = r.xn[rows, :].astype(f32)
            scale = r.scale_v[pl.ds(pl.multiple_of(k * sub, sub), sub), pl.ds(0, 1)]
            r.xn[rows, :] = (x * scale * r.gain_v[...]).astype(bf16)

    mark("p_barrier")
    pl.semaphore_wait(barrier, inner + outer - 1)
    send_tok = remote(r.xn.at[own, :], r.xn.at[own, :], r.tok_send, r.tok_recv, partner)
    send_tok.start()

    mark("p_kown")
    wk_copy.wait()
    r.yk[own, :] = nn(r.xn[own, :], r.wk_v[...]).astype(bf16)
    mark("p_vown")
    for copy in wv_copies:
        copy.wait()
    r.yv[own, :] = nn(r.xn[own, :], r.wv_v[...]).astype(bf16)
    mark("p_qown")
    wq_copy.wait()
    r.yq[own, :] = nn(r.xn[own, :], r.wq_v[...]).astype(bf16)
    mark("p_waittok")
    for copy in small[1:]:
        copy.wait()
    send_tok.wait()

    def log_decay_of(bias):
        return -jnp.log1p(jnp.exp(-(bias + math.log(sp_count * span / 8.0)))) / decay_power

    steps = (lax.broadcasted_iota(jnp.int32, (span, HEAD_K), 0) + (s * span + 1)).astype(f32)

    def values_of(h):
        return pl.ds(h * HEAD_V, HEAD_V)

    def keys_of(h):
        return pl.ds(h * HEAD_K, HEAD_K)

    mark("p_ktheir")
    r.yk[theirs, :] = nn(r.xn[theirs, :], r.wk_v[...]).astype(bf16)
    for h in range(heads):
        row = log_decay_of(r.bias_v[pl.ds(h, 1), :])
        r.kin[:, keys_of(h)] = (r.yk[:, keys_of(h)].astype(f32) * jnp.exp(-row * steps)).astype(
            bf16
        )

    def send_states(g):
        for d in range(1, inner):
            i = lax.rem(p + d, inner)
            remote(
                r.st_send.at[g, i], r.st_recv.at[g, d], r.a_send.at[g], r.a_recv.at[g], plane_dev(i)
            ).start()
        r.st_recv[g, 0] = r.st_send[g, p]

    for g in range(groups):
        mark(f"p_v{g}")
        cols = pl.ds(g * vcols, vcols)
        r.yv[theirs, cols] = nn(r.xn[theirs, :], r.wv_v[:, cols]).astype(bf16)
        for hh in range(pair):
            h = g * pair + hh
            state = tn(r.kin[:, keys_of(h)], r.yv[:, values_of(h)]).astype(bf16)
            for lane in range(HEAD_V // LANES):
                tiles = HEAD_K // PIECE_ROWS
                r.st_send[g, pl.ds(lane * tiles, tiles), hh] = state[
                    :, lane * LANES : (lane + 1) * LANES
                ].reshape(tiles, PIECE_ROWS, LANES)
        mark(f"p_asend{g}")
        send_states(g)

    mark("p_qtheir")
    r.yq[theirs, :] = nn(r.xn[theirs, :], r.wq_v[...]).astype(bf16)

    def gates(rows):
        u = nn(r.xn[rows, :], r.wg_v[...]).astype(bf16).astype(f32)
        r.sg[rows, :] = r.hgain_v[...] * (u * (0.5 + 0.5 * jnp.tanh(0.5 * u)))

    mark("p_gown")
    for copy in wg_copies:
        copy.wait()
    gates(own)

    def bulk(ref, ssem, rsem):
        return remote(ref, ref, ssem, rsem, partner)

    def b_copy(g, d):
        return remote(
            r.tot_send.at[g],
            r.tot_recv.at[g, d],
            r.b_send.at[g, d],
            r.b_recv.at[g, d],
            outer_dev(lax.rem(z + d, outer)),
        )

    for g in range(groups):
        mark(f"p_waitA{g}")
        bulk(r.st_recv.at[g, pl.ds(1, inner - 1)], r.a_send.at[g], r.a_recv.at[g]).wait_recv()
        mark(f"p_bsend{g}")
        total = r.st_recv[g, 0].astype(f32)
        for d in range(1, inner):
            total = total + r.st_recv[g, d].astype(f32)
        r.tot_send[g] = total.astype(bf16)
        for d in range(1, outer):

            @pl.when(z + d < outer)
            def _():
                b_copy(g, d).start()

    mark("p_gtheir")
    gates(theirs)

    mark("p_attn")
    for h in range(heads):
        row = log_decay_of(r.bias_v[pl.ds(h, 1), :])
        q_here = (
            r.yq[:, keys_of(h)].astype(f32) * (jnp.exp(row * steps) * HEAD_K ** (-0.5))
        ).astype(bf16)
        r.qin[:, keys_of(h)] = q_here
        v_here = r.yv[:, values_of(h)]
        parts = 2
        rows = span // parts
        for part in range(parts):
            last = (part + 1) * rows
            scores = nt(q_here[part * rows : last], r.kin[pl.ds(0, last), keys_of(h)])
            at = lax.broadcasted_iota(jnp.int32, scores.shape, 0) + part * rows
            to = lax.broadcasted_iota(jnp.int32, scores.shape, 1)
            scores = jnp.where(to <= at, scores, 0.0).astype(bf16)
            r.pv[pl.ds(part * rows, rows), values_of(h)] = nn(scores, v_here[:last])

    for g in range(groups):
        mark(f"p_waitB{g}")
        r.acc[...] = jnp.zeros_like(r.acc)
        for d in range(1, outer):

            @pl.when(z >= d)
            def _():
                b_copy(g, d).wait_recv()
                r.acc[...] += r.tot_recv[g, d].astype(f32)

        mark(f"p_csend{g}")
        carry = r.acc[...]
        for i in range(inner):
            r.c_send[g, i] = carry.astype(bf16)
            if i + 1 < inner:
                carry = carry + r.st_recv[g, lax.rem(p - i + inner, inner)].astype(f32)
        for d in range(1, inner):
            i = lax.rem(p + d, inner)
            remote(
                r.c_send.at[g, i], r.c_recv.at[g, p], r.cs_send.at[g], r.cs_recv.at[g], plane_dev(i)
            ).start()
        r.c_recv[g, p] = r.c_send[g, p]

    for g in range(groups):
        mark(f"p_waitC{g}")
        bulk(r.c_recv.at[g, pl.ds(1, inner - 1)], r.cs_send.at[g], r.cs_recv.at[g]).wait_recv()
        mark(f"p_fin{g}")
        for hh in range(pair):
            h = g * pair + hh
            tiles = HEAD_K // PIECE_ROWS
            state = jnp.concatenate(
                [
                    r.c_recv[g, pl.ds(lane * tiles, tiles), hh].reshape(HEAD_K, LANES)
                    for lane in range(HEAD_V // LANES)
                ],
                axis=1,
            )
            att = r.pv[:, values_of(h)] + nn(r.qin[:, keys_of(h)], state)
            scale = lax.rsqrt(jnp.mean(att * att, axis=-1, keepdims=True) + epsilon)
            r.gated[:, values_of(h)] = (att * scale * r.sg[:, values_of(h)]).astype(bf16)

    tiles = model // OUT_TILE

    def o_copy(t):
        return remote(r.o_send.at[t], r.o_recv.at[t], r.os_send.at[t], r.os_recv.at[t], partner)

    def out_copy(t):
        columns = pl.ds(t * OUT_TILE, OUT_TILE)
        return pltpu.make_async_copy(r.o_buf.at[t], r.out.at[:, columns], r.ob_sem.at[t])

    mark("p_otheirs")
    wo_copy.wait()
    for t in range(tiles):
        columns = pl.ds(t * OUT_TILE, OUT_TILE)
        r.o_send[t] = nn(r.gated[theirs, :], r.wo_v[:, columns]).astype(bf16)
        o_copy(t).start()
    mark("p_oown")
    for t in range(tiles):
        columns = pl.ds(t * OUT_TILE, OUT_TILE)
        part = nn(r.gated[own, :], r.wo_v[:, columns])
        o_copy(t).wait_recv()
        r.o_buf[t] = (part + r.o_recv[t].astype(f32)).astype(bf16)
        out_copy(t).start()

    mark("p_outwait")
    for t in range(tiles):
        o_copy(t).wait_send()
        out_copy(t).wait()
    for g in range(groups):
        bulk(r.st_send.at[g, pl.ds(1, inner - 1)], r.a_send.at[g], r.a_recv.at[g]).wait_send()
        bulk(r.c_send.at[g, pl.ds(1, inner - 1)], r.cs_send.at[g], r.cs_recv.at[g]).wait_send()
        for d in range(1, outer):

            @pl.when(z + d < outer)
            def _():
                b_copy(g, d).wait_send()

    mark(None)


def per_device(sp_count, tokens, norm_gain, wq, wk, wv, wg, decay_bias, head_gain, wo):
    half, model = tokens.shape
    span = 2 * half
    width = wk.shape[1]
    vwidth = wv.shape[1]
    heads = width // HEAD_K
    groups = 2
    pair = heads // groups
    outer = sp_count // PIECES
    tiles = model // OUT_TILE
    piece = (pair, PIECE_ROWS, LANES)
    vm = pltpu.VMEM
    dma = pltpu.SemaphoreType.DMA
    hbm = pl.BlockSpec(memory_space=pltpu.HBM)
    inputs = dict(
        tokens=tokens,
        norm_gain=norm_gain.reshape(1, model),
        wq=wq,
        wk=wk,
        wv=wv,
        wg=wg,
        decay_bias=decay_bias.reshape(heads, HEAD_K),
        head_gain=head_gain.reshape(1, vwidth),
        wo=wo,
    )
    scratch = dict(
        xn=vm((span, model), bf16),
        scale_v=vm((half // TOKEN_CHUNKS, LANES), f32),
        gain_v=vm((1, model), f32),
        bias_v=vm((heads, HEAD_K), f32),
        hgain_v=vm((1, vwidth), f32),
        wk_v=vm((model, width), bf16),
        wq_v=vm((model, width), bf16),
        wv_v=vm((model, vwidth), bf16),
        wg_v=vm((model, vwidth), bf16),
        wo_v=vm((vwidth, model), bf16),
        yk=vm((span, width), bf16),
        yq=vm((span, width), bf16),
        yv=vm((span, vwidth), bf16),
        sg=vm((span, vwidth), f32),
        kin=vm((span, width), bf16),
        qin=vm((span, width), bf16),
        pv=vm((span, vwidth), f32),
        gated=vm((span, vwidth), bf16),
        st_send=vm((groups, PIECES) + piece, bf16),
        st_recv=vm((groups, PIECES) + piece, bf16),
        tot_send=vm((groups,) + piece, bf16),
        tot_recv=vm((groups, outer) + piece, bf16),
        acc=vm(piece, f32),
        c_send=vm((groups, PIECES) + piece, bf16),
        c_recv=vm((groups, PIECES) + piece, bf16),
        o_send=vm((tiles, half, OUT_TILE), bf16),
        o_recv=vm((tiles, half, OUT_TILE), bf16),
        o_buf=vm((tiles, half, OUT_TILE), bf16),
        tok_sem=dma((TOKEN_CHUNKS,)),
        small_sem=dma((3,)),
        w_sem=dma((2 + 2 * groups,)),
        wo_sem=dma,
        tok_send=dma,
        tok_recv=dma,
        a_send=dma((groups,)),
        a_recv=dma((groups,)),
        b_send=dma((groups, outer)),
        b_recv=dma((groups, outer)),
        cs_send=dma((groups,)),
        cs_recv=dma((groups,)),
        os_send=dma((tiles,)),
        os_recv=dma((tiles,)),
        ob_sem=dma((tiles,)),
    )
    names = tuple(inputs) + ("out",) + tuple(scratch)
    return pl.pallas_call(
        functools.partial(kernel, sp_count, names),
        out_shape=jax.ShapeDtypeStruct((half, model), bf16),
        in_specs=[hbm] * len(inputs),
        out_specs=hbm,
        scratch_shapes=list(scratch.values()),
        compiler_params=pltpu.CompilerParams(
            collective_id=0, has_side_effects=True, vmem_limit_bytes=VMEM_BYTES
        ),
    )(*inputs.values())


def solution(mesh):
    return jax.shard_map(
        functools.partial(per_device, mesh.shape["sp"]),
        mesh=mesh,
        in_specs=(
            P(("sp", "tp"), None),
            P(),
            P(None, "tp"),
            P(None, "tp"),
            P(None, "tp"),
            P(None, "tp"),
            P("tp"),
            P("tp"),
            P("tp", None),
        ),
        out_specs=P(("sp", "tp"), None),
        check_vma=False,
    )
```

```python
import functools
import math
import types

import jax
import jax.numpy as jnp
from jax import lax
from jax.experimental import pallas as pl
from jax.experimental.pallas import tpu as pltpu
from jax.sharding import PartitionSpec as P

HEAD_K = 128
HEAD_V = 256
PIECES = 16
PIECE_ROWS = 16
LANES = 128

epsilon = 1e-06
decay_power = 16.0
MESH = pl.DeviceIdType.MESH
f32 = jnp.float32
bf16 = jnp.bfloat16
TOKEN_CHUNKS = 4
SEND_CHUNKS = 2
VMEM_BYTES = 62_500_000


def nn(a, b):
    return jnp.dot(a, b, preferred_element_type=f32)


def nt(a, b):
    return lax.dot_general(a, b, (((1,), (1,)), ((), ())), preferred_element_type=f32)


def tn(a, b):
    return lax.dot_general(a, b, (((0,), (0,)), ((), ())), preferred_element_type=f32)


def mark(name):
    pass


def kernel(sp_count, names, *refs):
    r = types.SimpleNamespace(**dict(zip(names, refs, strict=True)))
    s = lax.axis_index("sp")
    c = lax.axis_index("tp")
    other = 1 - c
    half, model = r.tokens.shape
    span = 2 * half
    heads = r.wk.shape[1] // HEAD_K
    groups = 2
    pair = heads // groups
    vcols = pair * HEAD_V
    inner = PIECES
    outer = sp_count // inner
    z = s // inner
    p = lax.rem(s, inner)

    own = pl.ds(pl.multiple_of(c * half, half), half)
    theirs = pl.ds(pl.multiple_of(other * half, half), half)
    partner = {"sp": s, "tp": other}

    def plane_dev(i):
        return {"sp": z * inner + i, "tp": c}

    def outer_dev(k):
        return {"sp": k * inner + p, "tp": c}

    def remote(src, dst, ssem, rsem, device):
        return pltpu.make_async_remote_copy(
            src_ref=src,
            dst_ref=dst,
            send_sem=ssem,
            recv_sem=rsem,
            device_id=device,
            device_id_type=MESH,
        )

    chunk = half // TOKEN_CHUNKS
    tok_copies = []
    for i in range(TOKEN_CHUNKS):
        rows = pl.ds(i * chunk, chunk)
        tok_copies.append(
            pltpu.make_async_copy(r.tokens.at[rows, :], r.xraw.at[rows, :], r.tok_sem.at[i])
        )
    small = [
        pltpu.make_async_copy(r.norm_gain, r.gain_v, r.small_sem.at[0]),
        pltpu.make_async_copy(r.decay_bias, r.bias_v, r.small_sem.at[1]),
        pltpu.make_async_copy(r.head_gain, r.hgain_v, r.small_sem.at[2]),
    ]
    wk_copy = pltpu.make_async_copy(r.wk, r.wk_v, r.w_sem.at[0])
    wq_copy = pltpu.make_async_copy(r.wq, r.wq_v, r.w_sem.at[1])
    wv_copies, wg_copies = [], []
    for g in range(groups):
        cols = pl.ds(g * vcols, vcols)
        wv_copies.append(
            pltpu.make_async_copy(r.wv.at[:, cols], r.wv_v.at[:, cols], r.w_sem.at[2 + g])
        )
        wg_copies.append(
            pltpu.make_async_copy(
                r.wg.at[:, cols], r.wg_v.at[:, cols], r.w_sem.at[2 + groups + g]
            )
        )
    wo_copy = pltpu.make_async_copy(r.wo, r.wo_v, r.wo_sem)
    for copy in tok_copies + small[:1]:
        copy.start()

    barrier = pltpu.get_barrier_semaphore()
    pl.semaphore_signal(barrier, inc=1, device_id=partner, device_id_type=MESH)
    for d in range(1, inner):
        pl.semaphore_signal(
            barrier, inc=1, device_id=plane_dev(lax.rem(p + d, inner)), device_id_type=MESH
        )
    for d in range(1, outer):
        pl.semaphore_signal(
            barrier, inc=1, device_id=outer_dev(lax.rem(z + d, outer)), device_id_type=MESH
        )

    wk_copy.start()
    mark("p_norm")
    sub = 16
    small[0].wait()
    for i in range(TOKEN_CHUNKS):
        tok_copies[i].wait()
        if i + 1 == TOKEN_CHUNKS:
            for copy in wv_copies + small[1:]:
                copy.start()

        @pl.loop(0, chunk // sub, unroll=True)
        def _(k):
            x = r.xraw[pl.ds(i * chunk + k * sub, sub), :].astype(f32)
            scale = lax.rsqrt(jnp.mean(x * x, axis=-1, keepdims=True) + epsilon)
            rows = pl.ds(pl.multiple_of(c * half + i * chunk + k * sub, sub), sub)
            r.xn[rows, :] = (x * scale * r.gain_v[...]).astype(bf16)

    mark("p_barrier")
    pl.semaphore_wait(barrier, inner + outer - 1)
    part_rows = half // SEND_CHUNKS
    tok_sends = []
    for i in range(SEND_CHUNKS):
        rows = pl.ds(pl.multiple_of(c * half + i * part_rows, part_rows), part_rows)
        tok_sends.append(
            remote(r.xn.at[rows, :], r.xn.at[rows, :], r.tok_send.at[i], r.tok_recv.at[i], partner)
        )
        tok_sends[-1].start()
    mark("p_kown")
    wk_copy.wait()
    r.yk[own, :] = nn(r.xn[own, :], r.wk_v[...]).astype(bf16)
    mark("p_vown")
    for copy in small[1:]:
        copy.wait()
    for g in range(groups):
        cols = pl.ds(g * vcols, vcols)
        wv_copies[g].wait()
        r.yv[own, cols] = nn(r.xn[own, :], r.wv_v[:, cols]).astype(bf16)
    for copy in [wq_copy] + wg_copies + [wo_copy]:
        copy.start()
    mark("p_stown")

    def log_decay_of(bias):
        return -jnp.log1p(jnp.exp(-(bias + math.log(sp_count * span / 8.0)))) / decay_power

    steps = (lax.broadcasted_iota(jnp.int32, (span, HEAD_K), 0) + (s * span + 1)).astype(f32)

    def values_of(h):
        return pl.ds(h * HEAD_V, HEAD_V)

    def keys_of(h):
        return pl.ds(h * HEAD_K, HEAD_K)

    def decayed_keys(rows, h):
        row = log_decay_of(r.bias_v[pl.ds(h, 1), :])
        first = (s * span + 1 + (c if rows is own else other) * half).astype(f32)
        steps_here = lax.broadcasted_iota(jnp.int32, (half, HEAD_K), 0).astype(f32) + first
        keys = r.yk[rows, keys_of(h)].astype(f32) * jnp.exp(-row * steps_here)
        r.kin[rows, keys_of(h)] = keys.astype(bf16)
        return tn(keys.astype(bf16), r.yv[rows, values_of(h)])

    for h in range(heads):
        r.st_acc[h] = decayed_keys(own, h)
    mark("p_waittok")
    for copy in tok_sends:
        copy.wait_recv()

    def send_states(g):
        for d in range(1, inner):
            i = lax.rem(p + d, inner)
            remote(
                r.st_send.at[g, i], r.st_recv.at[g, d], r.a_send.at[g], r.a_recv.at[g], plane_dev(i)
            ).start()
        r.st_recv[g, 0] = r.st_send[g, p]

    mark("p_ktheir")
    r.yk[theirs, :] = nn(r.xn[theirs, :], r.wk_v[...]).astype(bf16)
    for g in range(groups):
        mark(f"p_kv{g}")
        vcols_g = pl.ds(g * vcols, vcols)
        r.yv[theirs, vcols_g] = nn(r.xn[theirs, :], r.wv_v[:, vcols_g]).astype(bf16)
        for hh in range(pair):
            h = g * pair + hh
            state = (r.st_acc[h] + decayed_keys(theirs, h)).astype(bf16)
            for lane in range(HEAD_V // LANES):
                tiles = HEAD_K // PIECE_ROWS
                r.st_send[g, pl.ds(lane * tiles, tiles), hh] = state[
                    :, lane * LANES : (lane + 1) * LANES
                ].reshape(tiles, PIECE_ROWS, LANES)
        mark(f"p_asend{g}")
        send_states(g)

    def gates(rows, g):
        cols = pl.ds(g * vcols, vcols)
        u = nn(r.xn[rows, :], r.wg_v[:, cols]).astype(bf16).astype(f32)
        r.sg[rows, cols] = r.hgain_v[:, cols] * (u * (0.5 + 0.5 * jnp.tanh(0.5 * u)))

    def bulk(ref, ssem, rsem):
        return remote(ref, ref, ssem, rsem, partner)

    def b_copy(g, d):
        return remote(
            r.tot_send.at[g],
            r.tot_recv.at[g, d],
            r.b_send.at[g, d],
            r.b_recv.at[g, d],
            outer_dev(lax.rem(z + d, outer)),
        )

    def reduce_states(g):
        mark(f"p_waitA{g}")
        bulk(r.st_recv.at[g, pl.ds(1, inner - 1)], r.a_send.at[g], r.a_recv.at[g]).wait_recv()
        mark(f"p_bsend{g}")
        total = r.st_recv[g, 0].astype(f32)
        for d in range(1, inner):
            total = total + r.st_recv[g, d].astype(f32)
        r.tot_send[g] = total.astype(bf16)
        for d in range(1, outer):

            @pl.when(z + d < outer)
            def _():
                b_copy(g, d).start()

    def local_part(h):
        row = log_decay_of(r.bias_v[pl.ds(h, 1), :])
        q_here = (
            r.yq[:, keys_of(h)].astype(f32) * (jnp.exp(row * steps) * HEAD_K ** (-0.5))
        ).astype(bf16)
        r.qin[:, keys_of(h)] = q_here
        v_here = r.yv[:, values_of(h)]
        parts = 2
        rows = span // parts
        for part in range(parts):
            last = (part + 1) * rows
            scores = nt(q_here[part * rows : last], r.kin[pl.ds(0, last), keys_of(h)])
            at = lax.broadcasted_iota(jnp.int32, scores.shape, 0) + part * rows
            to = lax.broadcasted_iota(jnp.int32, scores.shape, 1)
            scores = jnp.where(to <= at, scores, 0.0).astype(bf16)
            r.pv[pl.ds(part * rows, rows), values_of(h)] = nn(scores, v_here[:last])

    def send_carries(g):
        mark(f"p_waitB{g}")
        r.acc[...] = jnp.zeros_like(r.acc)
        for d in range(1, outer):

            @pl.when(z >= d)
            def _():
                b_copy(g, d).wait_recv()
                r.acc[...] += r.tot_recv[g, d].astype(f32)

        mark(f"p_csend{g}")
        carry = r.acc[...]
        for i in range(inner):
            r.c_send[g, i] = carry.astype(bf16)
            if i + 1 < inner:
                carry = carry + r.st_recv[g, lax.rem(p - i + inner, inner)].astype(f32)
        for d in range(1, inner):
            i = lax.rem(p + d, inner)
            remote(
                r.c_send.at[g, i], r.c_recv.at[g, p], r.cs_send.at[g], r.cs_recv.at[g], plane_dev(i)
            ).start()
        r.c_recv[g, p] = r.c_send[g, p]

    def finish_heads(g):
        mark(f"p_waitC{g}")
        bulk(r.c_recv.at[g, pl.ds(1, inner - 1)], r.cs_send.at[g], r.cs_recv.at[g]).wait_recv()
        mark(f"p_fin{g}")
        for hh in range(pair):
            h = g * pair + hh
            tiles = HEAD_K // PIECE_ROWS
            state = jnp.concatenate(
                [
                    r.c_recv[g, pl.ds(lane * tiles, tiles), hh].reshape(HEAD_K, LANES)
                    for lane in range(HEAD_V // LANES)
                ],
                axis=1,
            )
            att = r.pv[:, values_of(h)] + nn(r.qin[:, keys_of(h)], state)
            scale = lax.rsqrt(jnp.mean(att * att, axis=-1, keepdims=True) + epsilon)
            r.gated[:, values_of(h)] = (att * scale * r.sg[:, values_of(h)]).astype(bf16)

    mark("p_q")
    wq_copy.wait()
    r.yq[...] = nn(r.xn[...], r.wq_v[...]).astype(bf16)
    mark("p_g0own")
    wg_copies[0].wait()
    gates(own, 0)
    reduce_states(0)
    mark("p_g1own")
    wg_copies[1].wait()
    gates(own, 1)
    reduce_states(1)
    mark("p_g0their")
    gates(theirs, 0)
    mark("p_attn0")
    for h in range(pair):
        local_part(h)
    send_carries(0)
    mark("p_g1their")
    gates(theirs, 1)
    send_carries(1)
    mark("p_attn1")
    for h in range(pair, heads):
        local_part(h)
    wo_copy.wait()

    finish_heads(0)
    mark("p_o0")
    low = pl.ds(0, vcols)
    high = pl.ds(vcols, vcols)
    r.part_t[...] = nn(r.gated[theirs, low], r.wo_v[low, :])
    r.part_o[...] = nn(r.gated[own, low], r.wo_v[low, :])
    finish_heads(1)
    ncols = model // 2

    def o_copy(n):
        dst = r.recv0 if n == 0 else r.recv1
        return remote(r.xraw.at[:, pl.ds(n * ncols, ncols)], dst, r.os_send.at[n], r.os_recv.at[n], partner)

    for n in range(2):
        mark(f"p_otheirs{n}")
        columns = pl.ds(n * ncols, ncols)
        r.xraw[:, columns] = (
            r.part_t[:, columns] + nn(r.gated[theirs, high], r.wo_v[high, columns])
        ).astype(bf16)
        o_copy(n).start()
    mark("p_oown")
    left = pl.ds(0, ncols)
    right = pl.ds(ncols, ncols)
    r.part_o[:, left] += nn(r.gated[own, high], r.wo_v[high, left])
    mark("p_wait0")
    o_copy(0).wait_recv()
    mark("p_oown1")
    r.part1[...] = r.part_o[:, right] + nn(r.gated[own, high], r.wo_v[high, right])
    r.res0[...] = (r.part_o[:, left] + r.recv0[...].astype(f32)).astype(bf16)
    mark("p_wait1")
    o_copy(1).wait_recv()
    mark("p_drain")
    for n in range(2):
        o_copy(n).wait_send()
    for copy in tok_sends:
        copy.wait_send()
    for g in range(groups):
        bulk(r.st_send.at[g, pl.ds(1, inner - 1)], r.a_send.at[g], r.a_recv.at[g]).wait_send()
        bulk(r.c_send.at[g, pl.ds(1, inner - 1)], r.cs_send.at[g], r.cs_recv.at[g]).wait_send()
        for d in range(1, outer):

            @pl.when(z + d < outer)
            def _():
                b_copy(g, d).wait_send()

    mark(None)


def write_out(res0, part1, recv1, out, buf, sem):
    cols = res0.shape[1]
    left = pltpu.make_async_copy(res0, out.at[:, pl.ds(0, cols)], sem.at[0])
    right = pltpu.make_async_copy(buf, out.at[:, pl.ds(cols, cols)], sem.at[1])
    left.start()
    buf[...] = (part1[...] + recv1[...].astype(f32)).astype(bf16)
    right.start()
    left.wait()
    right.wait()


def per_device(sp_count, tokens, norm_gain, wq, wk, wv, wg, decay_bias, head_gain, wo):
    half, model = tokens.shape
    span = 2 * half
    width = wk.shape[1]
    vwidth = wv.shape[1]
    heads = width // HEAD_K
    groups = 2
    pair = heads // groups
    outer = sp_count // PIECES
    piece = (pair, PIECE_ROWS, LANES)
    vm = pltpu.VMEM
    dma = pltpu.SemaphoreType.DMA
    hbm = pl.BlockSpec(memory_space=pltpu.HBM)
    inputs = dict(
        tokens=tokens,
        norm_gain=norm_gain.reshape(1, model),
        wq=wq,
        wk=wk,
        wv=wv,
        wg=wg,
        decay_bias=decay_bias.reshape(heads, HEAD_K),
        head_gain=head_gain.reshape(1, vwidth),
        wo=wo,
    )
    scratch = dict(
        xn=vm((span, model), bf16),
        xraw=vm((half, model), bf16),
        gain_v=vm((1, model), f32),
        bias_v=vm((heads, HEAD_K), f32),
        hgain_v=vm((1, vwidth), f32),
        wk_v=vm((model, width), bf16),
        wq_v=vm((model, width), bf16),
        wv_v=vm((model, vwidth), bf16),
        wg_v=vm((model, vwidth), bf16),
        wo_v=vm((vwidth, model), bf16),
        yk=vm((span, width), bf16),
        yq=vm((span, width), bf16),
        yv=vm((span, vwidth), bf16),
        sg=vm((span, vwidth), f32),
        kin=vm((span, width), bf16),
        qin=vm((span, width), bf16),
        pv=vm((span, vwidth), f32),
        gated=vm((span, vwidth), bf16),
        st_send=vm((groups, PIECES) + piece, bf16),
        st_recv=vm((groups, PIECES) + piece, bf16),
        tot_send=vm((groups,) + piece, bf16),
        tot_recv=vm((groups, outer) + piece, bf16),
        acc=vm(piece, f32),
        c_send=vm((groups, PIECES) + piece, bf16),
        c_recv=vm((groups, PIECES) + piece, bf16),
        st_acc=vm((heads, HEAD_K, HEAD_V), f32),
        recv0=vm((half, model // 2), bf16),
        part_t=vm((half, model), f32),
        part_o=vm((half, model), f32),
        tok_sem=dma((TOKEN_CHUNKS,)),
        small_sem=dma((3,)),
        w_sem=dma((2 + 2 * groups,)),
        wo_sem=dma,
        tok_send=dma((SEND_CHUNKS,)),
        tok_recv=dma((SEND_CHUNKS,)),
        a_send=dma((groups,)),
        a_recv=dma((groups,)),
        b_send=dma((groups, outer)),
        b_recv=dma((groups, outer)),
        cs_send=dma((groups,)),
        cs_recv=dma((groups,)),
        os_send=dma((2,)),
        os_recv=dma((2,)),
    )
    outs = dict(
        res0=vm((half, model // 2), bf16),
        part1=vm((half, model // 2), f32),
        recv1=vm((half, model // 2), bf16),
    )
    names = tuple(inputs) + tuple(outs) + tuple(scratch)
    vmem = pl.BlockSpec(memory_space=pltpu.VMEM)
    parts = pl.pallas_call(
        functools.partial(kernel, sp_count, names),
        out_shape=tuple(outs.values()),
        in_specs=[hbm] * len(inputs),
        out_specs=(vmem,) * len(outs),
        scratch_shapes=list(scratch.values()),
        compiler_params=pltpu.CompilerParams(
            collective_id=0, has_side_effects=True, vmem_limit_bytes=VMEM_BYTES
        ),
    )(*inputs.values())
    return pl.pallas_call(
        write_out,
        out_shape=jax.ShapeDtypeStruct((half, model), bf16),
        in_specs=[vmem] * len(outs),
        out_specs=hbm,
        scratch_shapes=[vm((half, model // 2), bf16), dma((2,))],
        compiler_params=pltpu.CompilerParams(vmem_limit_bytes=16_000_000),
    )(*[pltpu.with_memory_space_constraint(x, pltpu.VMEM) for x in parts])


def solution(mesh):
    return jax.shard_map(
        functools.partial(per_device, mesh.shape["sp"]),
        mesh=mesh,
        in_specs=(
            P(("sp", "tp"), None),
            P(),
            P(None, "tp"),
            P(None, "tp"),
            P(None, "tp"),
            P(None, "tp"),
            P("tp"),
            P("tp"),
            P("tp", None),
        ),
        out_specs=P(("sp", "tp"), None),
        check_vma=False,
    )
```
